32 devices in a mesh: sp: 4 (over y, core), dp: 8 (over z, x).
Axes of the slice: x: 2, y: 2, z: 4, core: 2. Of those that a mesh axis runs over, the one named last changes fastest.
Arguments:
- query_rows: bfloat16 [8, 512, 4, 128], P('dp', 'sp'), may hold values from -6 to 6
- key_rows: bfloat16 [8, 512, 4, 128], P('dp', 'sp'), may hold values from -6 to 6
- value_rows: bfloat16 [8, 512, 4, 128], P('dp', 'sp'), may hold values from -6 to 6
- map_weight: float32 [4], P('sp'), may hold values from 0.3 to 0.8
- head_gain: float32 [128], replicated, may hold values from 0.1 to 1.9
Outputs:
- mixed: bfloat16 [8, 512, 4, 128], P('dp', 'sp')
The draws below stay inside these ranges and needn't reach their ends.
All inputs are finite; a program needn't handle non-finite values.
Results may differ from the reference program's by a relative error of at most 0.0049.
Values may be sent and summed in bfloat16 or wider, within the bound.
No kernel may reach another device: no remote copies, remote signals or barrier semaphores. Data moves between devices by JAX's collectives and lax.ppermute only.
A program may use at most 64 MiB of HBM per device.

```python
import math
import jax
import jax.numpy as jnp
from jax import lax

QK = 64
VD = 128
SEGMENT = 64
HEADS = 4
SEQ_LEN = 512
SEQS = 8


def drawn_pair(key):
    shape = (SEQS, SEQ_LEN, HEADS, 2 * QK)
    query_draw = 1.3 * jax.random.truncated_normal(jax.random.fold_in(key, 11), -4.5, 4.5, shape, jnp.float32)
    key_draw = 1.3 * jax.random.truncated_normal(jax.random.fold_in(key, 12), -4.5, 4.5, shape, jnp.float32)
    return (query_draw, key_draw)


def draw_query_rows(key, part):
    return drawn_pair(key)[0].astype(jnp.bfloat16)


def draw_key_rows(key, part):
    return drawn_pair(key)[1].astype(jnp.bfloat16)


def block_scale(key, extent, shards, low, top_value):
    def one(dim, blocks):
        steps = jax.random.uniform(jax.random.fold_in(jax.random.fold_in(key, 6), dim), (blocks,), jnp.float32, low / len(shards), top_value / len(shards))
        return jnp.repeat(jnp.exp(steps), extent[dim] // blocks).reshape((-1,) + (1,) * (len(extent) - dim - 1))

    loudness = one(*shards[0])
    for cut in shards[1:]:
        loudness = loudness * one(*cut)
    return loudness


def gaussian(rng, shape, deviation, limit, cuts=(), kind=jnp.bfloat16):
    drawn = deviation * jax.random.normal(rng, shape, jnp.float32)
    if cuts:
        drawn = drawn * block_scale(rng, shape, cuts, -0.22, 0.18)
    return jnp.clip(drawn, -limit, limit).astype(kind)


def setup_inputs(seed: int = 0) -> dict:
    seeds = jax.random.split(jax.random.key(seed), 6)
    query_rows = draw_query_rows(jax.random.fold_in(seeds[5], 71), 0)
    key_rows = draw_key_rows(jax.random.fold_in(seeds[5], 71), 0)
    value_rows = gaussian(seeds[2], (SEQS, SEQ_LEN, HEADS, VD), 1.0, 6.0, ((0, 8), (1, 4)))
    map_weight = jnp.clip(0.3 + 0.5 * jax.random.uniform(seeds[3], (HEADS,), jnp.float32) ** block_scale(seeds[3], (HEADS,), ((0, 4),), -0.2, 0.2), 0.3, 0.8)
    head_gain = jnp.clip(1.0 + 0.18 * jax.random.normal(seeds[4], (VD,), jnp.float32), 0.1, 1.9)
    return dict(query_rows=query_rows, key_rows=key_rows, value_rows=value_rows, map_weight=map_weight, head_gain=head_gain)


def attend_head(query_head, key_head, value_head, weight_two, head_gain):
    length = key_head.shape[0]
    block_len = math.gcd(length, 512)
    key_segment = jnp.arange(length, dtype=jnp.int32) // SEGMENT

    def one_block(start):
        query_block = lax.dynamic_slice_in_dim(query_head, start, block_len, 0)
        query_segment = (start + jnp.arange(block_len, dtype=jnp.int32)) // SEGMENT
        visible = key_segment[None, :] <= query_segment[:, None]
        parts = []
        for which in range(2):
            query_map = query_block[:, which * QK:(which + 1) * QK]
            key_map = key_head[:, which * QK:(which + 1) * QK]
            scores = jnp.dot(query_map, key_map.T, preferred_element_type=jnp.float32) * QK ** (-0.5)
            scores = jnp.where(visible, scores, -jnp.inf)
            scores = scores - lax.optimization_barrier(jnp.max(scores, axis=-1, keepdims=True))
            raised = jnp.exp(scores)
            weights = raised / lax.optimization_barrier(jnp.sum(raised, axis=-1, keepdims=True))
            parts.append(jnp.dot(weights.astype(jnp.bfloat16), value_head, preferred_element_type=jnp.float32))
        attended = parts[0] - weight_two * parts[1]
        mean_square = lax.optimization_barrier(jnp.mean(attended * attended, axis=-1, keepdims=True))
        return (attended * lax.rsqrt(mean_square + 1e-06) * head_gain).astype(jnp.bfloat16)
    starts = jnp.arange(length // block_len, dtype=jnp.int32) * block_len
    return lax.map(one_block, starts).reshape(length, value_head.shape[1])

def reference(query_rows, key_rows, value_rows, map_weight, head_gain):

    def per_sequence(items):
        query_seq, key_seq, value_seq = items
        result = lax.map(lambda group: attend_head(group[0], group[1], group[2], group[3], head_gain), (query_seq.transpose(1, 0, 2), key_seq.transpose(1, 0, 2), value_seq.transpose(1, 0, 2), map_weight))
        return result.transpose(1, 0, 2)
    return lax.map(per_sequence, (query_rows, key_rows, value_rows))
```

```python
import functools
import math

import jax
import jax.numpy as jnp
from jax import lax
from jax.experimental import pallas as pl
from jax.experimental.pallas import tpu as pltpu
from jax.sharding import PartitionSpec as P

QK = 64
SEGMENT = 64
CORES = 2
EXP_SCALE = math.log2(math.e) * QK ** (-0.5)
SPARE_BYTES = 8 << 20
NT = (((1,), (1,)), ((), ()))


def each_head(heads, body):
    if heads <= 8:
        for head in range(heads):
            body(head)
    else:
        lax.fori_loop(0, heads, lambda head, c: (body(head), c)[1], 0)


def sources(peers):
    here = lax.axis_index("sp")
    cores = CORES if peers % CORES == 0 else 1
    chips = peers // cores
    chip, core = here // cores, here % cores
    straight = [lax.rem(chip + chips - r, chips) * cores + core for r in range(chips)]
    crossed = [lax.rem(chip + chips - r, chips) * cores + cores - 1 - core for r in range(chips)]
    if cores == 1:
        return here, [here], straight[1:], []
    return here, [here, crossed[0]], straight[1:], crossed[1:]


def head_rows(ref, head, heads, tokens):
    return ref[pl.ds(head, tokens, stride=heads), :].astype(jnp.bfloat16)


def hide(scores, here, source, tokens):
    queries = here * tokens + lax.rem(lax.broadcasted_iota(jnp.int32, scores.shape, 0), tokens)
    keys = source * tokens + lax.broadcasted_iota(jnp.int32, scores.shape, 1)
    return jnp.where(keys // SEGMENT <= queries // SEGMENT, scores, -jnp.inf)


def weigh(stacked, key_refs, srcs, here, head, heads, tokens, floor):
    scores = []
    for ref, source in zip(key_refs, srcs):
        block = lax.dot_general(stacked, head_rows(ref, head, heads, tokens), NT, preferred_element_type=jnp.float32)
        scores.append(hide(block, here, source, tokens))
    top = functools.reduce(jnp.maximum, scores)
    top = jnp.max(top, axis=1, keepdims=True)
    top = jnp.broadcast_to(top, scores[0].shape)
    if floor is not None:
        top = jnp.maximum(top, floor)
    raised = [jnp.exp2((block - top) * EXP_SCALE) for block in scores]
    total = jnp.sum(functools.reduce(jnp.add, raised), axis=1, keepdims=True)
    return top, raised, jnp.broadcast_to(total, scores[0].shape)


def widen(refs, wide):
    for i, ref in enumerate(refs):
        wide[i] = ref[...].astype(jnp.float32)
    return [wide.at[i] for i in range(len(refs))]


def near_scores(peers, heads, tokens, query, *refs):
    keys, (stacked, raised, top, total, wide) = refs[:-5], refs[-5:]
    here, near, _, _ = sources(peers)
    query_wide, *keys_wide = widen((query, *keys), wide)

    def body(head):
        rows = head_rows(query_wide, head, heads, tokens)
        first = lax.broadcasted_iota(jnp.int32, rows.shape, 1) < QK
        zero = jnp.zeros_like(rows)
        both = jnp.concatenate([jnp.where(first, rows, zero), jnp.where(first, zero, rows)], axis=0)
        stacked[head] = both
        peak, blocks, mass = weigh(both, keys_wide, near, here, head, heads, tokens, None)
        top[head] = peak
        total[head] = mass
        for i, block in enumerate(blocks):
            raised[i, head] = block

    each_head(heads, body)


def straight_scores(peers, heads, tokens, stacked, floor, *refs):
    keys, (raised, top, total, wide) = refs[:-4], refs[-4:]
    here, _, straight, _ = sources(peers)
    keys_wide = widen(keys, wide)

    def body(head):
        peak, blocks, mass = weigh(stacked[head], keys_wide, straight, here, head, heads, tokens, floor[head])
        top[head] = peak
        total[head] = mass
        for i, block in enumerate(blocks):
            raised[i, head] = block

    each_head(heads, body)


def last_scores(peers, heads, tokens, counts, *refs):
    refs = list(refs)
    stacked, near_raised, near_top, near_total, far_raised, far_top, far_total = refs[:7]
    n_near, n_straight, n_crossed = counts
    at = 7
    map_weights, at = refs[at : at + n_near + n_straight + n_crossed], at + n_near + n_straight + n_crossed
    values, at = refs[at : at + n_near + n_straight], at + n_near + n_straight
    keys, at = refs[at : at + n_crossed], at + n_crossed
    weights, partial, wide, values_wide = refs[at:]
    here, near, straight, crossed = sources(peers)
    keys_wide = widen(keys, wide)
    value_refs = widen(values, values_wide)
    per_peer = heads // peers

    def body(head):
        second = jnp.zeros((1, 1), jnp.float32)
        for ref, source in zip(map_weights, near + straight + crossed):
            for own in range(per_peer):
                second += jnp.where(source * per_peer + own == head, ref[:, own : own + 1], 0.0)
        peak, blocks, mass = weigh(stacked[head], keys_wide, crossed, here, head, heads, tokens, far_top[head])
        near_scale = jnp.exp2((near_top[head] - peak) * EXP_SCALE)
        far_scale = jnp.exp2((far_top[head] - peak) * EXP_SCALE)
        inverse = 1.0 / (near_scale * near_total[head] + far_scale * far_total[head] + mass)
        inverse = jnp.concatenate([inverse[:tokens], -second * inverse[tokens:]], axis=0)
        near_scale = near_scale * inverse
        far_scale = far_scale * inverse

        def joined(block, scale):
            scaled = block * scale
            return (scaled[:tokens] + scaled[tokens:]).astype(jnp.bfloat16)

        for i, block in enumerate(blocks):
            weights[i, head] = joined(block, inverse)
        ready = [joined(near_raised[i, head], near_scale) for i in range(n_near)]
        ready += [joined(far_raised[i, head], far_scale) for i in range(n_straight)]
        acc = None
        for weight, ref in zip(ready, value_refs):
            part = jnp.dot(weight, head_rows(ref, head, heads, tokens), preferred_element_type=jnp.float32)
            acc = part if acc is None else acc + part
        partial[head] = acc

    each_head(heads, body)


def finish(heads, tokens, weights, partial, gain, *refs):
    values, (out, wide, out_wide) = refs[:-3], refs[-3:]
    value_refs = widen(values, wide)

    def body(head):
        attended = partial[head]
        for i, ref in enumerate(value_refs):
            attended += jnp.dot(weights[i, head], head_rows(ref, head, heads, tokens), preferred_element_type=jnp.float32)
        mean_square = jnp.mean(attended * attended, axis=1, keepdims=True)
        out_wide[pl.ds(head, tokens, stride=heads), :] = attended * lax.rsqrt(mean_square + 1e-06) * gain[...]

    each_head(heads, body)
    out[...] = out_wide[...].astype(out.dtype)


def kernel(body, outs, scratch, vmem_out=True):
    space = pl.BlockSpec(memory_space=pltpu.VMEM)
    limit = SPARE_BYTES + sum(4 * math.prod(s.shape) for s in scratch)

    def call(*args):
        args = [pltpu.with_memory_space_constraint(a, pltpu.VMEM) if a.size > 1024 else a for a in args]
        return pl.pallas_call(
            body,
            out_shape=outs,
            in_specs=[space] * len(args),
            out_specs=jax.tree.map(lambda _: space, outs),
            scratch_shapes=scratch,
            compiler_params=pltpu.CompilerParams(vmem_limit_bytes=limit),
        )(*args)

    return call


def on_device(query_rows, key_rows, value_rows, map_weight, head_gain):
    peers = lax.axis_size("sp")
    _, tokens, heads, width = query_rows.shape
    cores = CORES if peers % CORES == 0 else 1
    chips = peers // cores
    rows = tokens * heads

    def turn(x, by):
        return lax.ppermute(x, "sp", [(i, (i + by * cores) % peers) for i in range(peers)])

    def swap(x):
        return lax.ppermute(x, "sp", [(i, i // cores * cores + cores - 1 - i % cores) for i in range(peers)])

    def flat(x):
        return x.reshape(rows, width)

    shift = range(1, chips)
    key_far = [turn(key_rows, r) for r in shift]
    value_far = [turn(value_rows, r) for r in shift]
    weight_far = [turn(map_weight, r) for r in shift]
    crossing = cores > 1
    key_near = [key_rows] + ([swap(key_rows)] if crossing else [])
    value_near = [value_rows] + ([swap(value_rows)] if crossing else [])
    weight_near = [map_weight] + ([swap(map_weight)] if crossing else [])
    key_last = [swap(x) for x in key_far] if crossing else []
    value_last = [swap(x) for x in value_far] if crossing else []
    weight_last = [swap(x) for x in weight_far] if crossing else []
    n_near, n_far, n_last = len(key_near), len(key_far), len(key_last)

    f32 = lambda *s: jax.ShapeDtypeStruct(s, jnp.float32)
    bf16 = lambda *s: jax.ShapeDtypeStruct(s, jnp.bfloat16)
    wide = lambda n: pltpu.VMEM((n, rows, width), jnp.float32)
    stat = f32(heads, 2 * tokens, tokens)
    blocks = lambda n: f32(n, heads, 2 * tokens, tokens)

    stacked, near_raised, near_top, near_total = kernel(
        functools.partial(near_scores, peers, heads, tokens),
        (bf16(heads, 2 * tokens, width), blocks(n_near), stat, stat),
        [wide(1 + n_near)],
    )(flat(query_rows), *map(flat, key_near))
    far_raised, far_top, far_total = kernel(
        functools.partial(straight_scores, peers, heads, tokens),
        (blocks(n_far), stat, stat),
        [wide(n_far)],
    )(stacked, near_top, *map(flat, key_far))
    weights, partial = kernel(
        functools.partial(last_scores, peers, heads, tokens, (n_near, n_far, n_last)),
        (bf16(n_last, heads, tokens, tokens), f32(heads, tokens, width)),
        [wide(n_last), wide(n_near + n_far)],
    )(
        stacked, near_raised, near_top, near_total, far_raised, far_top, far_total,
        *(w.reshape(1, -1) for w in weight_near + weight_far + weight_last),
        *map(flat, value_near + value_far),
        *map(flat, key_last),
    )
    mixed = kernel(
        functools.partial(finish, heads, tokens),
        bf16(rows, width),
        [wide(n_last), pltpu.VMEM((rows, width), jnp.float32)],
    )(weights, partial, head_gain.reshape(1, -1), *map(flat, value_last))
    return mixed.reshape(query_rows.shape)


def solution(mesh):
    rows = P("dp", "sp", None, None)
    return jax.shard_map(
        on_device,
        mesh=mesh,
        in_specs=(rows, rows, rows, P("sp"), P()),
        out_specs=rows,
        check_vma=False,
    )
```

```python
import functools
import math

import jax
import jax.numpy as jnp
from jax import lax
from jax.experimental import pallas as pl
from jax.experimental.pallas import tpu as pltpu
from jax.sharding import PartitionSpec as P

QK = 64
SEGMENT = 64
CORES = 2
EXP_SCALE = math.log2(math.e) * QK ** (-0.5)
SPARE_BYTES = 2 << 20
NT = (((1,), (1,)), ((), ()))


def each_head(heads, body):
    if heads <= 8:
        for head in range(heads):
            body(head)
    else:
        lax.fori_loop(0, heads, lambda head, c: (body(head), c)[1], 0)


def sources(peers):
    here = lax.axis_index("sp")
    cores = CORES if peers % CORES == 0 else 1
    chips = peers // cores
    chip, core = here // cores, here % cores
    straight = [lax.rem(chip + chips - r, chips) * cores + core for r in range(chips)]
    crossed = [lax.rem(chip + chips - r, chips) * cores + cores - 1 - core for r in range(chips)]
    if cores == 1:
        return here, [here], straight[1:], []
    return here, [here, crossed[0]], straight[1:], crossed[1:]


def widen(refs, wide):
    for i, ref in enumerate(refs):
        wide[i] = ref[...].astype(jnp.float32)
    return [wide.at[i] for i in range(len(refs))]


def split_rows(ref, head, heads, tokens):
    return ref[pl.ds(head, tokens, stride=heads), :].astype(jnp.bfloat16)


def head_rows(ref, head, tokens):
    return ref[pl.ds(head * tokens, tokens), :]


def hide(scores, here, source, tokens):
    queries = here * tokens + lax.rem(lax.broadcasted_iota(jnp.int32, scores.shape, 0), tokens)
    keys = source * tokens + lax.broadcasted_iota(jnp.int32, scores.shape, 1)
    return jnp.where(keys // SEGMENT <= queries // SEGMENT, scores, -jnp.inf)


def weigh(stacked, keys, srcs, here, tokens, floor):
    scores = [
        hide(lax.dot_general(stacked, key, NT, preferred_element_type=jnp.float32), here, source, tokens)
        for key, source in zip(keys, srcs)
    ]
    top = jnp.max(functools.reduce(jnp.maximum, scores), axis=1, keepdims=True)
    top = jnp.broadcast_to(top, scores[0].shape)
    if floor is not None:
        top = jnp.maximum(top, floor)
    raised = [jnp.exp2((block - top) * EXP_SCALE) for block in scores]
    total = jnp.sum(functools.reduce(jnp.add, raised), axis=1, keepdims=True)
    return top, raised, jnp.broadcast_to(total, scores[0].shape)


def weighted(blocks, values):
    return functools.reduce(
        jnp.add, [jnp.dot(block, value, preferred_element_type=jnp.float32) for block, value in zip(blocks, values)]
    )


def spread(map_weight, tile):
    for own in range(tile.shape[0]):
        tile[own] = jnp.full(tile.shape[1:], map_weight[own])


def prepare(heads, tokens, query, key, value, gain, stacked, key_heads, value_heads, gain_tile, wide):
    query_wide, key_wide, value_wide = widen((query, key, value), wide)

    def body(head):
        rows = split_rows(query_wide, head, heads, tokens)
        first = lax.broadcasted_iota(jnp.int32, rows.shape, 1) < QK
        zero = jnp.zeros_like(rows)
        stacked[head] = jnp.concatenate([jnp.where(first, rows, zero), jnp.where(first, zero, rows)], axis=0)
        key_heads[pl.ds(head * tokens, tokens), :] = split_rows(key_wide, head, heads, tokens)
        value_heads[pl.ds(head * tokens, tokens), :] = split_rows(value_wide, head, heads, tokens)

    each_head(heads, body)
    gain_tile[...] = jnp.broadcast_to(gain[...], gain_tile.shape)


def near_scores(peers, heads, tokens, stacked, key_heads, *refs):
    keys, (raised, top, total, wide) = refs[:-4], refs[-4:]
    here, near, _, _ = sources(peers)
    keys_wide = widen(keys, wide)

    def body(head):
        blocks = [head_rows(key_heads, head, tokens)] + [split_rows(ref, head, heads, tokens) for ref in keys_wide]
        top[head], blocks, total[head] = weigh(stacked[head], blocks, near, here, tokens, None)
        for i, block in enumerate(blocks):
            raised[i, head] = block.astype(jnp.bfloat16)

    each_head(heads, body)


def straight_scores(peers, heads, tokens, counts, stacked, near_raised, floor, value_heads, *refs):
    here, _, straight, _ = sources(peers)
    n_side, n_near = counts
    values, keys = refs[:n_side], refs[n_side:-6]
    raised, top, total, summed, wide, value_wide = refs[-6:]
    keys_wide = widen(keys, wide)
    values_wide = widen(values, value_wide)

    def body(head):
        blocks = [split_rows(ref, head, heads, tokens) for ref in keys_wide]
        top[head], blocks, total[head] = weigh(stacked[head], blocks, straight, here, tokens, floor[head])
        for i, block in enumerate(blocks):
            raised[i, head] = block.astype(jnp.bfloat16)
        near_values = [head_rows(value_heads, head, tokens)] + [split_rows(v, head, heads, tokens) for v in values_wide]
        summed[head] = weighted([near_raised[i, head] for i in range(n_near)], near_values)

    each_head(heads, body)


def last_scores(peers, heads, tokens, stacked, summed, near_top, near_total, far_raised, far_top, far_total, *refs):
    here, _, straight, crossed = sources(peers)
    values, keys = refs[: len(straight)], refs[len(straight) : -4]
    weights, partial, wide, value_wide = refs[-4:]
    keys_wide = widen(keys, wide)
    values_wide = widen(values, value_wide)

    def body(head):
        blocks = [split_rows(ref, head, heads, tokens) for ref in keys_wide]
        peak, blocks, mass = weigh(stacked[head], blocks, crossed, here, tokens, far_top[head])
        near_scale = jnp.exp2((near_top[head] - peak) * EXP_SCALE)
        far_scale = jnp.exp2((far_top[head] - peak) * EXP_SCALE)
        inverse = 1.0 / (near_scale * near_total[head] + far_scale * far_total[head] + mass)
        for i, block in enumerate(blocks):
            weights[i, head] = (block * inverse).astype(jnp.bfloat16)
        far_values = [split_rows(v, head, heads, tokens) for v in values_wide]
        far = weighted([far_raised[i, head] for i in range(len(straight))], far_values)
        partial[head] = (summed[head] * near_scale + far * far_scale) * inverse

    each_head(heads, body)


def write_rows(attended, head, heads, tokens, gain, out_wide):
    mean_square = jnp.mean(attended * attended, axis=1, keepdims=True)
    out_wide[pl.ds(head, tokens, stride=heads), :] = attended * lax.rsqrt(mean_square + 1e-06) * gain[0:1, :]


def owned(head, per_peer, tiles, order):
    second = jnp.zeros((1, tiles[0].shape[-1]), jnp.float32)
    for tile, source in zip(tiles, order):
        for own in range(per_peer):
            second += jnp.where(source * per_peer + own == head, tile[own, 0:1, :], 0.0)
    return second


def finish(peers, heads, tokens, weights, partial, gain, *refs):
    _, near, straight, crossed = sources(peers)
    order = near + straight + crossed
    tiles, values, (out, wide, out_wide) = refs[: len(order)], refs[len(order) : -3], refs[-3:]
    values_wide = widen(values, wide)

    def body(head):
        both = partial[head] + weighted(
            [weights[i, head] for i in range(len(values))], [split_rows(v, head, heads, tokens) for v in values_wide]
        )
        attended = both[:tokens] - owned(head, heads // peers, tiles, order) * both[tokens:]
        write_rows(attended, head, heads, tokens, gain, out_wide)

    each_head(heads, body)
    out[...] = out_wide[...].astype(out.dtype)


def kernel(body, outs, scratch, fetched=False):
    space = pl.BlockSpec(memory_space=pltpu.VMEM)
    held = sum(4 * math.prod(s.shape) for s in scratch)
    held += sum(math.prod(o.shape) * o.dtype.itemsize for o in jax.tree.leaves(outs))
    place = pltpu.HBM if fetched else pltpu.VMEM

    def call(*args):
        scalar = [a.ndim == 1 for a in args]
        limit = SPARE_BYTES + held
        if fetched:
            limit += sum(a.size * a.dtype.itemsize for a in args)
        args = [a if s else pltpu.with_memory_space_constraint(a, place) for a, s in zip(args, scalar)]
        return pl.pallas_call(
            body,
            out_shape=outs,
            in_specs=[pl.BlockSpec(memory_space=pltpu.SMEM) if s else space for s in scalar],
            out_specs=jax.tree.map(lambda _: space, outs),
            scratch_shapes=scratch,
            compiler_params=pltpu.CompilerParams(vmem_limit_bytes=limit),
        )(*args)

    return call


def on_device(query_rows, key_rows, value_rows, map_weight, head_gain):
    peers = lax.axis_size("sp")
    _, tokens, heads, width = query_rows.shape
    cores = CORES if peers % CORES == 0 else 1
    chips = peers // cores
    rows = tokens * heads

    def turn(x, by):
        return lax.ppermute(x, "sp", [(i, (i + by * cores) % peers) for i in range(peers)])

    def swap(x):
        return lax.ppermute(x, "sp", [(i, i // cores * cores + cores - 1 - i % cores) for i in range(peers)])

    def flat(x):
        return x.reshape(rows, width)

    f32 = lambda *s: jax.ShapeDtypeStruct(s, jnp.float32)
    bf16 = lambda *s: jax.ShapeDtypeStruct(s, jnp.bfloat16)
    wide = lambda n: pltpu.VMEM((n, rows, width), jnp.float32)
    both = (heads, 2 * tokens, tokens)
    shift = range(1, chips)
    n_near, n_far, n_last = cores, chips - 1, (chips - 1) * (cores - 1)

    key_far = [turn(key_rows, r) for r in shift]
    tile = kernel(spread, f32(heads // peers, 8, width), [])(map_weight)
    value_far = [turn(value_rows, r) for r in shift]
    weight_far = [turn(tile, r) for r in shift]
    key_near = [swap(key_rows)] if cores > 1 else []
    value_near = [swap(value_rows)] if cores > 1 else []
    weight_near = [tile] + ([swap(tile)] if cores > 1 else [])
    stacked, key_heads, value_heads, gain_tile = kernel(
        functools.partial(prepare, heads, tokens),
        (bf16(heads, 2 * tokens, width), bf16(rows, width), bf16(rows, width), f32(8, width)),
        [wide(3)],
        fetched=True,
    )(flat(query_rows), flat(key_rows), flat(value_rows), head_gain.reshape(1, -1))
    near_raised, near_top, near_total = kernel(
        functools.partial(near_scores, peers, heads, tokens),
        (bf16(n_near, *both), f32(*both), f32(*both)),
        [wide(max(cores - 1, 1))],
    )(stacked, key_heads, *map(flat, key_near))
    key_last = [swap(x) for x in key_far] if cores > 1 else []
    far_raised, far_top, far_total, summed = kernel(
        functools.partial(straight_scores, peers, heads, tokens, (cores - 1, n_near)),
        (bf16(n_far, *both), f32(*both), f32(*both), f32(heads, 2 * tokens, width)),
        [wide(n_far), wide(max(cores - 1, 1))],
    )(stacked, near_raised, near_top, value_heads, *map(flat, value_near), *map(flat, key_far))
    value_last = [swap(x) for x in value_far] if cores > 1 else []
    weight_last = [swap(x) for x in weight_far] if cores > 1 else []
    weights, partial = kernel(
        functools.partial(last_scores, peers, heads, tokens),
        (bf16(n_last, *both), f32(heads, 2 * tokens, width)),
        [wide(n_last), wide(n_far)],
    )(
        stacked, summed, near_top, near_total, far_raised, far_top, far_total,
        *map(flat, value_far), *map(flat, key_last),
    )
    mixed = kernel(
        functools.partial(finish, peers, heads, tokens),
        bf16(rows, width),
        [wide(n_last), pltpu.VMEM((rows, width), jnp.float32)],
    )(weights, partial, gain_tile, *weight_near, *weight_far, *weight_last, *map(flat, value_last))
    return mixed.reshape(query_rows.shape)


def solution(mesh):
    rows = P("dp", "sp", None, None)

    return jax.shard_map(
        on_device,
        mesh=mesh,
        in_specs=(rows, rows, rows, P("sp"), P()),
        out_specs=rows,
        check_vma=False,
    )
```

```python
import functools
import math

import jax
import jax.numpy as jnp
from jax import lax
from jax.experimental import pallas as pl
from jax.experimental.pallas import tpu as pltpu
from jax.sharding import PartitionSpec as P

QK = 64
SEGMENT = 64
CORES = 2
EXP_SCALE = math.log2(math.e) * QK ** (-0.5)
SPARE_BYTES = 2 << 20
NT = (((1,), (1,)), ((), ()))


def each_head(heads, body):
    if heads <= 8:
        for head in range(heads):
            body(head)
    else:
        lax.fori_loop(0, heads, lambda head, c: (body(head), c)[1], 0)


def sources(peers):
    here = lax.axis_index("sp")
    cores = CORES if peers % CORES == 0 else 1
    chips = peers // cores
    chip, core = here // cores, here % cores
    straight = [lax.rem(chip + chips - r, chips) * cores + core for r in range(chips)]
    crossed = [lax.rem(chip + chips - r, chips) * cores + cores - 1 - core for r in range(chips)]
    if cores == 1:
        return here, [here], straight[1:], []
    return here, [here, crossed[0]], straight[1:], crossed[1:]


def widen(refs, wide):
    for i, ref in enumerate(refs):
        wide[i] = ref[...].astype(jnp.float32)
    return [wide.at[i] for i in range(len(refs))]


def split_rows(ref, head, heads, tokens):
    return ref[pl.ds(head, tokens, stride=heads), :].astype(jnp.bfloat16)


def head_rows(ref, head, tokens):
    return ref[pl.ds(head * tokens, tokens), :]


def hide(scores, here, source, tokens):
    queries = here * tokens + lax.rem(lax.broadcasted_iota(jnp.int32, scores.shape, 0), tokens)
    keys = source * tokens + lax.broadcasted_iota(jnp.int32, scores.shape, 1)
    return jnp.where(keys // SEGMENT <= queries // SEGMENT, scores, -jnp.inf)


def weigh(stacked, keys, srcs, here, tokens, floor):
    scores = [
        hide(lax.dot_general(stacked, key, NT, preferred_element_type=jnp.float32), here, source, tokens)
        for key, source in zip(keys, srcs)
    ]
    top = jnp.max(functools.reduce(jnp.maximum, scores), axis=1, keepdims=True)
    top = jnp.broadcast_to(top, scores[0].shape)
    if floor is not None:
        top = jnp.maximum(top, floor)
    raised = [jnp.exp2((block - top) * EXP_SCALE) for block in scores]
    total = jnp.sum(functools.reduce(jnp.add, raised), axis=1, keepdims=True)
    return top, raised, jnp.broadcast_to(total, scores[0].shape)


def weighted(blocks, values):
    return functools.reduce(
        jnp.add, [jnp.dot(block, value, preferred_element_type=jnp.float32) for block, value in zip(blocks, values)]
    )


def prepare(heads, tokens, query, key, value, gain, stacked, key_heads, value_heads, gain_tile, wide):
    query_wide, key_wide, value_wide = widen((query, key, value), wide)

    def body(head):
        rows = split_rows(query_wide, head, heads, tokens)
        first = lax.broadcasted_iota(jnp.int32, rows.shape, 1) < QK
        zero = jnp.zeros_like(rows)
        stacked[head] = jnp.concatenate([jnp.where(first, rows, zero), jnp.where(first, zero, rows)], axis=0)
        key_heads[pl.ds(head * tokens, tokens), :] = split_rows(key_wide, head, heads, tokens)
        value_heads[pl.ds(head * tokens, tokens), :] = split_rows(value_wide, head, heads, tokens)

    each_head(heads, body)
    gain_tile[...] = jnp.broadcast_to(gain[...], gain_tile.shape)


def near_scores(peers, heads, tokens, stacked, key_heads, gain, *refs):
    here, near, _, _ = sources(peers)
    tiles, keys = refs[: len(near)], refs[len(near) : -6]
    raised, top, total, gain_out, pair, wide = refs[-6:]
    keys_wide = widen(keys, wide)
    gain_out[...] = gain[...]
    for i, tile in enumerate(tiles):
        pair[i] = tile[...]

    def body(head):
        blocks = [head_rows(key_heads, head, tokens)] + [split_rows(ref, head, heads, tokens) for ref in keys_wide]
        top[head], blocks, total[head] = weigh(stacked[head], blocks, near, here, tokens, None)
        for i, block in enumerate(blocks):
            raised[i, head] = block.astype(jnp.bfloat16)

    each_head(heads, body)


def straight_scores(peers, heads, tokens, counts, stacked, near_raised, floor, gain, pair, value_heads, *refs):
    here, _, straight, _ = sources(peers)
    n_side, n_near = counts
    values, keys = refs[:n_side], refs[n_side:-8]
    raised, top, total, summed, gain_out, pair_out, wide, value_wide = refs[-8:]
    gain_out[...] = gain[...]
    pair_out[...] = pair[...]
    keys_wide = widen(keys, wide)
    values_wide = widen(values, value_wide)

    def body(head):
        blocks = [split_rows(ref, head, heads, tokens) for ref in keys_wide]
        top[head], blocks, total[head] = weigh(stacked[head], blocks, straight, here, tokens, floor[head])
        for i, block in enumerate(blocks):
            raised[i, head] = block.astype(jnp.bfloat16)
        near_values = [head_rows(value_heads, head, tokens)] + [split_rows(v, head, heads, tokens) for v in values_wide]
        summed[head] = weighted([near_raised[i, head] for i in range(n_near)], near_values)

    each_head(heads, body)


def owned(head, per_peer, pairs, order):
    near, straight, crossed = order
    owners = [(pairs[0], i, source) for i, source in enumerate(near)]
    for pair, *both in zip(pairs[1:], straight, *([crossed] if crossed else [])):
        owners += [(pair, i, source) for i, source in enumerate(both)]
    second = jnp.zeros((1, pairs[0].shape[-1]), jnp.float32)
    for ref, i, source in owners:
        for own in range(per_peer):
            second += jnp.where(source * per_peer + own == head, ref[i, own, 0:1, :], 0.0)
    return second


def last_scores(peers, heads, tokens, stacked, summed, near_top, near_total, far_raised, far_top, far_total, *refs):
    here, _, straight, crossed = sources(peers)
    values, keys = refs[: len(straight)], refs[len(straight) : -4]
    weights, partial, wide, value_wide = refs[-4:]
    keys_wide = widen(keys, wide)
    values_wide = widen(values, value_wide)

    def body(head):
        blocks = [split_rows(ref, head, heads, tokens) for ref in keys_wide]
        peak, blocks, mass = weigh(stacked[head], blocks, crossed, here, tokens, far_top[head])
        near_scale = jnp.exp2((near_top[head] - peak) * EXP_SCALE)
        far_scale = jnp.exp2((far_top[head] - peak) * EXP_SCALE)
        inverse = 1.0 / (near_scale * near_total[head] + far_scale * far_total[head] + mass)
        for i, block in enumerate(blocks):
            weights[i, head] = (block * inverse).astype(jnp.bfloat16)
        far_values = [split_rows(v, head, heads, tokens) for v in values_wide]
        far = weighted([far_raised[i, head] for i in range(len(straight))], far_values)
        partial[head] = (summed[head] * near_scale + far * far_scale) * inverse

    each_head(heads, body)


def write_rows(attended, head, heads, tokens, gain, out_wide):
    mean_square = jnp.mean(attended * attended, axis=1, keepdims=True)
    out_wide[pl.ds(head, tokens, stride=heads), :] = attended * lax.rsqrt(mean_square + 1e-06) * gain[0:1, :]


def finish_near(peers, heads, tokens, summed, near_total, gain, *refs):
    pairs, (out, out_wide) = refs[:-2], refs[-2:]
    order = sources(peers)[1:]

    def body(head):
        both = summed[head] / near_total[head]
        attended = both[:tokens] - owned(head, heads // peers, pairs, order) * both[tokens:]
        write_rows(attended, head, heads, tokens, gain, out_wide)

    each_head(heads, body)
    out[...] = out_wide[...].astype(out.dtype)


def finish(peers, heads, tokens, weights, partial, gain, *refs):
    order = sources(peers)[1:]
    n_pairs = 1 + len(order[1])
    pairs, values, (out, wide, out_wide) = refs[:n_pairs], refs[n_pairs:-3], refs[-3:]
    values_wide = widen(values, wide)

    def body(head):
        both = partial[head] + weighted(
            [weights[i, head] for i in range(len(values))], [split_rows(v, head, heads, tokens) for v in values_wide]
        )
        attended = both[:tokens] - owned(head, heads // peers, pairs, order) * both[tokens:]
        write_rows(attended, head, heads, tokens, gain, out_wide)

    each_head(heads, body)
    out[...] = out_wide[...].astype(out.dtype)


def spread(map_weight, tile):
    for own in range(tile.shape[0]):
        tile[own] = jnp.full(tile.shape[1:], map_weight[own])


def hold(*refs):
    pass


def kernel(body, outs, scratch, fetched=False, keep=False):
    space = pl.BlockSpec(memory_space=pltpu.VMEM)
    held = sum(4 * math.prod(s.shape) for s in scratch if s.dtype == jnp.float32)
    held += sum(math.prod(o.shape) * o.dtype.itemsize for o in jax.tree.leaves(outs))

    def call(*args):
        limit = SPARE_BYTES + held
        if fetched:
            limit += sum(a.size * a.dtype.itemsize for a in args)
        if fetched or keep:
            args = [pltpu.with_memory_space_constraint(a, pltpu.HBM if fetched else pltpu.VMEM) for a in args]
        return pl.pallas_call(
            body,
            out_shape=outs,
            in_specs=[pl.BlockSpec(memory_space=pltpu.SMEM) if a.ndim == 1 else space for a in args],
            out_specs=jax.tree.map(lambda _: space, outs),
            scratch_shapes=scratch,
            input_output_aliases={i: i for i in range(len(args))} if keep else {},
            compiler_params=pltpu.CompilerParams(vmem_limit_bytes=limit),
        )(*args)

    return call


def on_device(query_rows, key_rows, value_rows, map_weight, head_gain):
    peers = lax.axis_size("sp")
    _, tokens, heads, width = query_rows.shape
    cores = CORES if peers % CORES == 0 else 1
    chips = peers // cores
    rows = tokens * heads

    def turn(x, by):
        return lax.ppermute(x, "sp", [(i, (i + by * cores) % peers) for i in range(peers)])

    def swap(x):
        return lax.ppermute(x, "sp", [(i, i // cores * cores + cores - 1 - i % cores) for i in range(peers)])

    def flat(x):
        return x.reshape(rows, width)

    f32 = lambda *s: jax.ShapeDtypeStruct(s, jnp.float32)
    bf16 = lambda *s: jax.ShapeDtypeStruct(s, jnp.bfloat16)
    wide = lambda n: pltpu.VMEM((n, rows, width), jnp.float32)
    both = (heads, 2 * tokens, tokens)
    shift = range(1, chips)
    n_near, n_far, n_last = cores, chips - 1, (chips - 1) * (cores - 1)

    key_far = [turn(key_rows, r) for r in shift]
    value_far = [turn(value_rows, r) for r in shift]
    tile = kernel(spread, f32(heads // peers, 8, width), [])(map_weight)
    tiles = [tile] + ([swap(tile)] if cores > 1 else [])
    key_near = [swap(key_rows)] if cores > 1 else []
    value_near = [swap(value_rows)] if cores > 1 else []
    stacked, key_heads, value_heads, gain_tile = kernel(
        functools.partial(prepare, heads, tokens),
        (bf16(heads, 2 * tokens, width), bf16(rows, width), bf16(rows, width), f32(8, width)),
        [wide(3)],
        fetched=True,
    )(flat(query_rows), flat(key_rows), flat(value_rows), head_gain.reshape(1, -1))
    near_raised, near_top, near_total, gain_tile, pair = kernel(
        functools.partial(near_scores, peers, heads, tokens),
        (bf16(n_near, *both), f32(*both), f32(*both), f32(8, width), f32(n_near, heads // peers, 8, width)),
        [wide(max(cores - 1, 1))],
    )(stacked, key_heads, gain_tile, *tiles, *map(flat, key_near))
    pairs = [pair] + [turn(pair, r) for r in shift]
    key_last = [swap(x) for x in key_far] if cores > 1 else []
    far_raised, far_top, far_total, summed, gain_tile, pair_tile = kernel(
        functools.partial(straight_scores, peers, heads, tokens, (cores - 1, n_near)),
        (bf16(n_far, *both), f32(*both), f32(*both), f32(heads, 2 * tokens, width), f32(8, width), f32(*pair.shape)),
        [wide(n_far), wide(max(cores - 1, 1))],
    )(stacked, near_raised, near_top, gain_tile, pair, value_heads, *map(flat, value_near), *map(flat, key_far))
    arrived = (*value_far, *key_last, *pairs[1:])
    arrived = kernel(hold, tuple(jax.ShapeDtypeStruct(x.shape, x.dtype) for x in arrived), [], keep=True)(*arrived)
    value_far, key_last, pairs = arrived[:n_far], arrived[n_far : n_far + n_last], [pair_tile, *arrived[n_far + n_last :]]

    def later_chip():
        value_last = [swap(x) for x in value_far] if cores > 1 else []
        weights, partial = kernel(
            functools.partial(last_scores, peers, heads, tokens),
            (bf16(n_last, *both), f32(heads, 2 * tokens, width)),
            [wide(n_last), wide(n_far)],
        )(
            stacked, summed, near_top, near_total, far_raised, far_top, far_total,
            *map(flat, value_far), *map(flat, key_last),
        )
        return kernel(
            functools.partial(finish, peers, heads, tokens),
            bf16(rows, width),
            [wide(n_last), pltpu.VMEM((rows, width), jnp.float32)],
        )(weights, partial, gain_tile, *pairs, *map(flat, value_last))

    def first_chip():
        return kernel(
            functools.partial(finish_near, peers, heads, tokens),
            bf16(rows, width),
            [pltpu.VMEM((rows, width), jnp.float32)],
        )(summed, near_total, gain_tile, *pairs)

    mixed = lax.cond(lax.axis_index("sp") >= cores, later_chip, first_chip)
    return mixed.reshape(query_rows.shape)


def solution(mesh):
    rows = P("dp", "sp", None, None)

    return jax.shard_map(
        on_device,
        mesh=mesh,
        in_specs=(rows, rows, rows, P("sp"), P()),
        out_specs=rows,
        check_vma=False,
    )
```

```python
import functools
import math

import jax
import jax.numpy as jnp
from jax import lax
from jax.experimental import pallas as pl
from jax.experimental.pallas import tpu as pltpu
from jax.sharding import PartitionSpec as P

QK = 64
SEGMENT = 64
CORES = 2
EXP_SCALE = math.log2(math.e) * QK ** (-0.5)
SPARE_BYTES = 2 << 20
PACK = 16
PARTS = 3
NT = (((1,), (1,)), ((), ()))


def each_head(heads, body):
    if heads <= 8:
        for head in range(heads):
            body(head)
    else:
        lax.fori_loop(0, heads, lambda head, c: (body(head), c)[1], 0)


def sources(peers):
    here = lax.axis_index("sp")
    cores = CORES if peers % CORES == 0 else 1
    chips = peers // cores
    chip, core = here // cores, here % cores
    straight = [lax.rem(chip + chips - r, chips) * cores + core for r in range(chips)]
    crossed = [lax.rem(chip + chips - r, chips) * cores + cores - 1 - core for r in range(chips)]
    if cores == 1:
        return here, [here], straight[1:], []
    return here, [here, crossed[0]], straight[1:], crossed[1:]


def widen(refs, wide):
    for i, ref in enumerate(refs):
        wide[i] = ref[...].astype(jnp.float32)
    return [wide.at[i] for i in range(len(refs))]


def split_rows(ref, head, heads, tokens):
    return ref[pl.ds(head, tokens, stride=heads), :].astype(jnp.bfloat16)


def head_rows(ref, head, tokens):
    return ref[pl.ds(head * tokens, tokens), :]


def hide(scores, here, source, tokens):
    queries = here * tokens + lax.rem(lax.broadcasted_iota(jnp.int32, scores.shape, 0), tokens)
    keys = source * tokens + lax.broadcasted_iota(jnp.int32, scores.shape, 1)
    return jnp.where(keys // SEGMENT <= queries // SEGMENT, scores, -jnp.inf)


def weigh(stacked, keys, srcs, here, tokens, floor):
    scores = [
        hide(lax.dot_general(stacked, key, NT, preferred_element_type=jnp.float32), here, source, tokens)
        for key, source in zip(keys, srcs)
    ]
    top = jnp.max(functools.reduce(jnp.maximum, scores), axis=1, keepdims=True)
    top = jnp.broadcast_to(top, scores[0].shape)
    if floor is not None:
        top = jnp.maximum(top, floor)
    raised = [jnp.exp2((block - top) * EXP_SCALE) for block in scores]
    total = jnp.sum(functools.reduce(jnp.add, raised), axis=1, keepdims=True)
    return top, raised, jnp.broadcast_to(total, scores[0].shape)


def weighted(blocks, values):
    return functools.reduce(
        jnp.add, [jnp.dot(block, value, preferred_element_type=jnp.float32) for block, value in zip(blocks, values)]
    )


def prepare(heads, tokens, query, key, value, gain, stacked, key_heads, value_heads, gain_tile, wide):
    query_wide, key_wide, value_wide = widen((query, key, value), wide)

    def body(head):
        rows = split_rows(query_wide, head, heads, tokens)
        first = lax.broadcasted_iota(jnp.int32, rows.shape, 1) < QK
        zero = jnp.zeros_like(rows)
        stacked[head] = jnp.concatenate([jnp.where(first, rows, zero), jnp.where(first, zero, rows)], axis=0)
        key_heads[pl.ds(head * tokens, tokens), :] = split_rows(key_wide, head, heads, tokens)
        value_heads[pl.ds(head * tokens, tokens), :] = split_rows(value_wide, head, heads, tokens)

    each_head(heads, body)
    gain_tile[...] = jnp.broadcast_to(gain[...], gain_tile.shape)


def pack(heads, tokens, key, value, key_pack, value_pack, wide):
    key_wide, value_wide = widen((key, value), wide)

    def body(head):
        key_pack[pl.ds(head * tokens, tokens), :] = split_rows(key_wide, head, heads, tokens)
        value_pack[pl.ds(head * tokens, tokens), :] = split_rows(value_wide, head, heads, tokens)

    each_head(heads, body)


def blank(key_pack, value_pack):
    for ref in (key_pack, value_pack):
        ref[...] = jnp.zeros_like(ref)


def stamp(rows, map_weight, value_in, value_pack, tile):
    value_pack[pl.ds(0, rows), :] = value_in[pl.ds(0, rows), :]
    for own in range(tile.shape[0]):
        rest = jnp.full((PACK, value_pack.shape[1]), map_weight[own])
        tile[own] = rest[: tile.shape[1]]
        row = lax.broadcasted_iota(jnp.int32, rest.shape, 0)
        packed = jnp.zeros_like(rest)
        for part in range(PARTS):
            piece = rest.astype(jnp.bfloat16).astype(jnp.float32)
            packed = jnp.where(row == part, piece, packed)
            rest = rest - piece
        value_pack[pl.ds(rows + own * PACK, PACK), :] = packed.astype(jnp.bfloat16)


def stamped(value_pack, rows, per_peer):
    found = []
    for own in range(per_peer):
        parts = value_pack[pl.ds(rows + own * PACK, PACK), :].astype(jnp.float32)
        found.append(sum(parts[i : i + 1] for i in range(PARTS)))
    return found


def near_scores(peers, heads, tokens, stacked, key_heads, gain, *refs):
    here, near, _, _ = sources(peers)
    tiles, keys = refs[: len(near)], refs[len(near) : -5]
    raised, level, gain_out, pair, wide = refs[-5:]
    keys_wide = widen(keys, wide)
    gain_out[...] = gain[...]
    for i, tile in enumerate(tiles):
        pair[i] = tile[...]

    def body(head):
        blocks = [head_rows(key_heads, head, tokens)] + [split_rows(ref, head, heads, tokens) for ref in keys_wide]
        peak, blocks, mass = weigh(stacked[head], blocks, near, here, tokens, None)
        inverse = 1.0 / mass
        level[head] = peak + jnp.log(mass) * QK**0.5
        for i, block in enumerate(blocks):
            raised[i, head] = (block * inverse).astype(jnp.bfloat16)

    each_head(heads, body)


def straight_scores(peers, heads, tokens, counts, stacked, near_raised, near_level, gain, pair, value_heads, *refs):
    here, _, straight, _ = sources(peers)
    n_side, n_near = counts
    values, keys = refs[:n_side], refs[n_side:-6]
    raised, level, summed, gain_out, pair_out, value_wide = refs[-6:]
    gain_out[...] = gain[...]
    pair_out[...] = pair[...]
    values_wide = widen(values, value_wide)

    def body(head):
        blocks = [head_rows(ref, head, tokens) for ref in keys]
        peak, blocks, mass = weigh(stacked[head], blocks, straight, here, tokens, near_level[head])
        prior = jnp.exp2((near_level[head] - peak) * EXP_SCALE)
        mass = prior + mass
        inverse = 1.0 / mass
        level[head] = peak + jnp.log(mass) * QK**0.5
        for i, block in enumerate(blocks):
            raised[i, head] = (block * inverse).astype(jnp.bfloat16)
        near_values = [head_rows(value_heads, head, tokens)] + [split_rows(v, head, heads, tokens) for v in values_wide]
        summed[head] = weighted([near_raised[i, head] for i in range(n_near)], near_values) * (prior * inverse)

    each_head(heads, body)


def owned(head, per_peer, here, held):
    second = jnp.zeros_like(held[0][0][0])
    for rows, source, by in held:
        for own in range(per_peer):
            here_too = source * per_peer + own == head
            if by is not None:
                here_too = jnp.logical_and(here_too, (source < here) if by == "pack" else (source > here))
            second += jnp.where(here_too, rows[own], 0.0)
    return second


def tile_rows(tiles, i, per_peer):
    return [tiles[i, own, 0:1, :] for own in range(per_peer)]


def by_pair(pairs, side, per_peer):
    straight, crossed = side
    found = [(tile_rows(pair, 0, per_peer), source, "pair") for pair, source in zip(pairs, straight)]
    return found + [(tile_rows(pair, 1, per_peer), source, "pair") for pair, source in zip(pairs, crossed)]


def last_scores(peers, heads, tokens, stacked, summed, level, far_raised, *refs):
    here, _, straight, crossed = sources(peers)
    values, keys, (weights, partial) = refs[: len(straight)], refs[len(straight) : -2], refs[-2:]

    def body(head):
        blocks = [head_rows(ref, head, tokens) for ref in keys]
        peak, blocks, mass = weigh(stacked[head], blocks, crossed, here, tokens, level[head])
        prior = jnp.exp2((level[head] - peak) * EXP_SCALE)
        inverse = 1.0 / (prior + mass)
        for i, block in enumerate(blocks):
            weights[i, head] = (block * inverse).astype(jnp.bfloat16)
        far_values = [head_rows(ref, head, tokens) for ref in values]
        far = weighted([far_raised[i, head] for i in range(len(straight))], far_values)
        partial[head] = (summed[head] + far) * (prior * inverse)

    each_head(heads, body)


def write_rows(attended, head, heads, tokens, gain, out_wide):
    mean_square = jnp.mean(attended * attended, axis=1, keepdims=True)
    out_wide[pl.ds(head, tokens, stride=heads), :] = attended * lax.rsqrt(mean_square + 1e-06) * gain[0:1, :]


def finish_near(peers, heads, tokens, summed, gain, near_pair, *refs):
    pairs, (out, out_wide) = refs[:-2], refs[-2:]
    here, near, *far = sources(peers)
    per_peer = heads // peers
    held = [(tile_rows(near_pair, i, per_peer), source, None) for i, source in enumerate(near)]
    held += by_pair(pairs, far, per_peer)

    def body(head):
        both = summed[head]
        attended = both[:tokens] - owned(head, per_peer, here, held) * both[tokens:]
        write_rows(attended, head, heads, tokens, gain, out_wide)

    each_head(heads, body)
    out[...] = out_wide[...].astype(out.dtype)


def finish(peers, heads, tokens, weights, partial, gain, near_pair, *refs):
    here, near, straight, crossed = sources(peers)
    ends = len(straight), len(straight) + len(crossed)
    far, last, pairs, (out, out_wide) = refs[: ends[0]], refs[ends[0] : ends[1]], refs[ends[1] : -2], refs[-2:]
    per_peer = heads // peers
    held = [(tile_rows(near_pair, i, per_peer), source, None) for i, source in enumerate(near)]
    for refs_in, side in ((far, straight), (last, crossed)):
        held += [(stamped(ref, heads * tokens, per_peer), source, "pack") for ref, source in zip(refs_in, side)]
    held += by_pair(pairs, (straight, crossed), per_peer) if pairs else []

    def body(head):
        both = partial[head] + weighted(
            [weights[i, head] for i in range(len(last))], [head_rows(ref, head, tokens) for ref in last]
        )
        attended = both[:tokens] - owned(head, per_peer, here, held) * both[tokens:]
        write_rows(attended, head, heads, tokens, gain, out_wide)

    each_head(heads, body)
    out[...] = out_wide[...].astype(out.dtype)


def hold(*refs):
    pass


def kernel(body, outs, scratch, fetched=False, keep=False, aliases=None):
    space = pl.BlockSpec(memory_space=pltpu.VMEM)
    held = sum(4 * math.prod(s.shape) for s in scratch if s.dtype == jnp.float32)
    held += sum(math.prod(o.shape) * o.dtype.itemsize for o in jax.tree.leaves(outs))

    def call(*args):
        limit = SPARE_BYTES + held + sum(a.size * a.dtype.itemsize for a in args)
        if fetched or keep:
            args = [pltpu.with_memory_space_constraint(a, pltpu.HBM if fetched else pltpu.VMEM) for a in args]
        return pl.pallas_call(
            body,
            out_shape=outs,
            in_specs=[pl.BlockSpec(memory_space=pltpu.SMEM) if a.ndim == 1 else space for a in args],
            out_specs=jax.tree.map(lambda _: space, outs),
            scratch_shapes=scratch,
            input_output_aliases={i: i for i in range(len(args))} if keep else aliases or {},
            compiler_params=pltpu.CompilerParams(vmem_limit_bytes=limit),
        )(*args)

    return call


def on_device(query_rows, key_rows, value_rows, map_weight, head_gain):
    peers = lax.axis_size("sp")
    _, tokens, heads, width = query_rows.shape
    cores = CORES if peers % CORES == 0 else 1
    chips = peers // cores
    rows = tokens * heads

    def turn(x, by):
        return lax.ppermute(x, "sp", [(i, (i + by * cores) % peers) for i in range(peers)])

    def swap(x):
        return lax.ppermute(x, "sp", [(i, i // cores * cores + cores - 1 - i % cores) for i in range(peers)])

    def flat(x):
        return x.reshape(rows, width)

    f32 = lambda *s: jax.ShapeDtypeStruct(s, jnp.float32)
    bf16 = lambda *s: jax.ShapeDtypeStruct(s, jnp.bfloat16)
    wide = lambda n: pltpu.VMEM((n, rows, width), jnp.float32)
    both = (heads, 2 * tokens, tokens)
    shift = range(1, chips)
    n_near, n_far, n_last = cores, chips - 1, (chips - 1) * (cores - 1)

    chip = lax.axis_index("sp") // cores
    packs = (bf16(rows, width), bf16(rows + heads // peers * PACK, width))

    def sender():
        return kernel(functools.partial(pack, heads, tokens), packs, [wide(2)])(flat(key_rows), flat(value_rows))

    def receiver():
        return kernel(blank, packs, [])()

    key_pack, value_pack = lax.cond(chip < chips - 1, sender, receiver)
    key_far = [turn(key_pack, r) for r in shift]
    value_pack, tile = kernel(
        functools.partial(stamp, rows), (packs[1], f32(heads // peers, 8, width)), [], aliases={1: 0}
    )(map_weight, value_pack)
    value_far = [turn(value_pack, r) for r in shift]
    tiles = [tile] + ([swap(tile)] if cores > 1 else [])
    key_near = [swap(key_rows)] if cores > 1 else []
    value_near = [swap(value_rows)] if cores > 1 else []
    stacked, key_heads, value_heads, gain_tile = kernel(
        functools.partial(prepare, heads, tokens),
        (bf16(heads, 2 * tokens, width), bf16(rows, width), bf16(rows, width), f32(8, width)),
        [wide(3)],
        fetched=True,
    )(flat(query_rows), flat(key_rows), flat(value_rows), head_gain.reshape(1, -1))
    near_raised, near_level, gain_tile, pair = kernel(
        functools.partial(near_scores, peers, heads, tokens),
        (bf16(n_near, *both), f32(*both), f32(8, width), f32(n_near, heads // peers, 8, width)),
        [wide(max(cores - 1, 1))],
    )(stacked, key_heads, gain_tile, *tiles, *map(flat, key_near))
    pairs = [turn(pair, r) for r in shift]
    key_last = [swap(x) for x in key_far] if cores > 1 else []
    far_raised, level, summed, gain_tile, pair_tile = kernel(
        functools.partial(straight_scores, peers, heads, tokens, (cores - 1, n_near)),
        (
            bf16(n_far, *both), f32(*both), f32(heads, 2 * tokens, width), f32(8, width), f32(*pair.shape),
        ),
        [wide(max(cores - 1, 1))],
    )(stacked, near_raised, near_level, gain_tile, pair, value_heads, *map(flat, value_near), *key_far)

    def stay(*arrays):
        return kernel(hold, tuple(jax.ShapeDtypeStruct(x.shape, x.dtype) for x in arrays), [], keep=True)(*arrays)

    middle = chips > 2
    arrived = stay(*value_far, *key_last, *(pairs if middle else ()))
    value_far, key_last, late = arrived[:n_far], arrived[n_far : n_far + n_last], arrived[n_far + n_last :]

    def later_chip():
        value_last = [swap(x) for x in value_far] if cores > 1 else []
        weights, partial = kernel(
            functools.partial(last_scores, peers, heads, tokens),
            (bf16(n_last, *both), f32(heads, 2 * tokens, width)),
            [],
        )(stacked, summed, level, far_raised, *value_far, *key_last)
        return kernel(
            functools.partial(finish, peers, heads, tokens),
            bf16(rows, width),
            [pltpu.VMEM((rows, width), jnp.float32)],
        )(weights, partial, gain_tile, pair_tile, *value_far, *value_last, *late)

    def no_rows():
        return kernel(hold, bf16(rows, width), [])()

    mixed = lax.cond(chip > 0, later_chip, no_rows)
    mixed, *pairs = stay(mixed, *pairs)

    def first_chip():
        return kernel(
            functools.partial(finish_near, peers, heads, tokens),
            bf16(rows, width),
            [pltpu.VMEM((rows, width), jnp.float32)],
        )(summed, gain_tile, pair_tile, *pairs)

    mixed = lax.cond(chip > 0, lambda: mixed, first_chip)
    return mixed.reshape(query_rows.shape)


def solution(mesh):
    rows = P("dp", "sp", None, None)

    return jax.shard_map(
        on_device,
        mesh=mesh,
        in_specs=(rows, rows, rows, P("sp"), P()),
        out_specs=rows,
        check_vma=False,
    )
```

```python
import functools
import math

import jax
import jax.numpy as jnp
from jax import lax
from jax.experimental import pallas as pl
from jax.experimental.pallas import tpu as pltpu
from jax.sharding import PartitionSpec as P

QK = 64
SEGMENT = 64
CORES = 2
EXP_SCALE = math.log2(math.e) * QK ** (-0.5)
SPARE_BYTES = 2 << 20
PACK = 16
PARTS = 3
NT = (((1,), (1,)), ((), ()))


def each_head(heads, body):
    if heads <= 8:
        for head in range(heads):
            body(head)
    else:
        lax.fori_loop(0, heads, lambda head, c: (body(head), c)[1], 0)


def sources(peers):
    here = lax.axis_index("sp")
    cores = CORES if peers % CORES == 0 else 1
    chips = peers // cores
    chip, core = here // cores, here % cores
    straight = [lax.rem(chip + chips - r, chips) * cores + core for r in range(chips)]
    crossed = [lax.rem(chip + chips - r, chips) * cores + cores - 1 - core for r in range(chips)]
    if cores == 1:
        return here, [here], straight[1:], []
    return here, [here, crossed[0]], straight[1:], crossed[1:]


def widen(refs, wide):
    for i, ref in enumerate(refs):
        wide[i] = ref[...].astype(jnp.float32)
    return [wide.at[i] for i in range(len(refs))]


def split_rows(ref, head, heads, tokens):
    return ref[pl.ds(head, tokens, stride=heads), :].astype(jnp.bfloat16)


def head_rows(ref, head, tokens):
    return ref[pl.ds(head * tokens, tokens), :]


def hide(scores, here, source, tokens):
    queries = here * tokens + lax.rem(lax.broadcasted_iota(jnp.int32, scores.shape, 0), tokens)
    keys = source * tokens + lax.broadcasted_iota(jnp.int32, scores.shape, 1)
    return jnp.where(keys // SEGMENT <= queries // SEGMENT, scores, -jnp.inf)


def weigh(stacked, keys, srcs, here, tokens, floor):
    scores = [
        hide(lax.dot_general(stacked, key, NT, preferred_element_type=jnp.float32), here, source, tokens)
        for key, source in zip(keys, srcs)
    ]
    top = jnp.max(functools.reduce(jnp.maximum, scores), axis=1, keepdims=True)
    top = jnp.broadcast_to(top, scores[0].shape)
    if floor is not None:
        top = jnp.maximum(top, floor)
    raised = [jnp.exp2((block - top) * EXP_SCALE) for block in scores]
    total = jnp.sum(functools.reduce(jnp.add, raised), axis=1, keepdims=True)
    return top, raised, jnp.broadcast_to(total, scores[0].shape)


def weighted(blocks, values):
    return functools.reduce(
        jnp.add, [jnp.dot(block, value, preferred_element_type=jnp.float32) for block, value in zip(blocks, values)]
    )


def prepare(heads, tokens, query, key, value, gain, stacked, key_heads, value_heads, gain_tile, wide):
    query_wide, key_wide, value_wide = widen((query, key, value), wide)

    def body(head):
        rows = split_rows(query_wide, head, heads, tokens)
        first = lax.broadcasted_iota(jnp.int32, rows.shape, 1) < QK
        zero = jnp.zeros_like(rows)
        stacked[head] = jnp.concatenate([jnp.where(first, rows, zero), jnp.where(first, zero, rows)], axis=0)
        key_heads[pl.ds(head * tokens, tokens), :] = split_rows(key_wide, head, heads, tokens)
        value_heads[pl.ds(head * tokens, tokens), :] = split_rows(value_wide, head, heads, tokens)

    each_head(heads, body)
    gain_tile[...] = jnp.broadcast_to(gain[...], gain_tile.shape)


def pack(heads, tokens, key, value, key_pack, value_pack, wide):
    key_wide, value_wide = widen((key, value), wide)

    def body(head):
        key_pack[pl.ds(head * tokens, tokens), :] = split_rows(key_wide, head, heads, tokens)
        value_pack[pl.ds(head * tokens, tokens), :] = split_rows(value_wide, head, heads, tokens)

    each_head(heads, body)


def blank(key_pack, value_pack):
    for ref in (key_pack, value_pack):
        ref[...] = jnp.zeros_like(ref)


def stamp(rows, map_weight, value_in, value_pack, tile):
    value_pack[pl.ds(0, rows), :] = value_in[pl.ds(0, rows), :]
    for own in range(tile.shape[0]):
        rest = jnp.full((PACK, value_pack.shape[1]), map_weight[own])
        tile[own] = rest[: tile.shape[1]]
        row = lax.broadcasted_iota(jnp.int32, rest.shape, 0)
        packed = jnp.zeros_like(rest)
        for part in range(PARTS):
            piece = rest.astype(jnp.bfloat16).astype(jnp.float32)
            packed = jnp.where(row == part, piece, packed)
            rest = rest - piece
        value_pack[pl.ds(rows + own * PACK, PACK), :] = packed.astype(jnp.bfloat16)


def stamped(value_pack, rows, per_peer):
    found = []
    for own in range(per_peer):
        parts = value_pack[pl.ds(rows + own * PACK, PACK), :].astype(jnp.float32)
        found.append(sum(parts[i : i + 1] for i in range(PARTS)))
    return found


def near_scores(peers, heads, tokens, stacked, key_heads, gain, *refs):
    here, near, _, _ = sources(peers)
    tiles, keys = refs[: len(near)], refs[len(near) : -5]
    raised, level, gain_out, pair, wide = refs[-5:]
    keys_wide = widen(keys, wide)
    gain_out[...] = gain[...]
    for i, tile in enumerate(tiles):
        pair[i] = tile[...]

    def body(head):
        blocks = [head_rows(key_heads, head, tokens)] + [split_rows(ref, head, heads, tokens) for ref in keys_wide]
        peak, blocks, mass = weigh(stacked[head], blocks, near, here, tokens, None)
        inverse = 1.0 / mass
        level[head] = peak + jnp.log(mass) * QK**0.5
        for i, block in enumerate(blocks):
            raised[i, head] = (block * inverse).astype(jnp.bfloat16)

    each_head(heads, body)


def straight_scores(peers, heads, tokens, counts, stacked, near_raised, near_level, gain, pair, value_heads, *refs):
    here, _, straight, _ = sources(peers)
    n_side, n_near = counts
    values, keys = refs[:n_side], refs[n_side:-6]
    raised, level, summed, gain_out, pair_out, value_wide = refs[-6:]
    gain_out[...] = gain[...]
    pair_out[...] = pair[...]
    values_wide = widen(values, value_wide)

    def body(head):
        blocks = [head_rows(ref, head, tokens) for ref in keys]
        peak, blocks, mass = weigh(stacked[head], blocks, straight, here, tokens, near_level[head])
        prior = jnp.exp2((near_level[head] - peak) * EXP_SCALE)
        mass = prior + mass
        inverse = 1.0 / mass
        level[head] = peak + jnp.log(mass) * QK**0.5
        for i, block in enumerate(blocks):
            raised[i, head] = (block * inverse).astype(jnp.bfloat16)
        near_values = [head_rows(value_heads, head, tokens)] + [split_rows(v, head, heads, tokens) for v in values_wide]
        summed[head] = weighted([near_raised[i, head] for i in range(n_near)], near_values) * (prior * inverse)

    each_head(heads, body)


def owned(head, per_peer, here, held):
    second = jnp.zeros_like(held[0][0][0])
    for rows, source, by in held:
        for own in range(per_peer):
            here_too = source * per_peer + own == head
            if by is not None:
                here_too = jnp.logical_and(here_too, (source < here) if by == "pack" else (source > here))
            second += jnp.where(here_too, rows[own], 0.0)
    return second


def tile_rows(tiles, i, per_peer):
    return [tiles[i, own, 0:1, :] for own in range(per_peer)]


def by_pair(pairs, side, per_peer):
    straight, crossed = side
    found = [(tile_rows(pair, 0, per_peer), source, "pair") for pair, source in zip(pairs, straight)]
    return found + [(tile_rows(pair, 1, per_peer), source, "pair") for pair, source in zip(pairs, crossed)]


def last_scores(peers, heads, tokens, stacked, summed, level, far_raised, near_pair, *refs):
    here, near, straight, crossed = sources(peers)
    values, keys, (weights, partial, second) = refs[: len(straight)], refs[len(straight) : -3], refs[-3:]
    per_peer = heads // peers
    held = [(tile_rows(near_pair, i, per_peer), source, None) for i, source in enumerate(near)]
    held += [(stamped(ref, heads * tokens, per_peer), source, "pack") for ref, source in zip(values, straight)]

    def body(head):
        second[head] = jnp.broadcast_to(owned(head, per_peer, here, held), second.shape[1:])
        blocks = [head_rows(ref, head, tokens) for ref in keys]
        peak, blocks, mass = weigh(stacked[head], blocks, crossed, here, tokens, level[head])
        prior = jnp.exp2((level[head] - peak) * EXP_SCALE)
        inverse = 1.0 / (prior + mass)
        for i, block in enumerate(blocks):
            weights[i, head] = (block * inverse).astype(jnp.bfloat16)
        far_values = [head_rows(ref, head, tokens) for ref in values]
        far = weighted([far_raised[i, head] for i in range(len(straight))], far_values)
        partial[head] = (summed[head] + far) * (prior * inverse)

    each_head(heads, body)


def write_rows(attended, head, heads, tokens, gain, out_wide):
    mean_square = jnp.mean(attended * attended, axis=1, keepdims=True)
    out_wide[pl.ds(head, tokens, stride=heads), :] = attended * lax.rsqrt(mean_square + 1e-06) * gain[0:1, :]


def finish_near(peers, heads, tokens, summed, gain, near_pair, *refs):
    pairs, (out, out_wide) = refs[:-2], refs[-2:]
    here, near, *far = sources(peers)
    per_peer = heads // peers
    held = [(tile_rows(near_pair, i, per_peer), source, None) for i, source in enumerate(near)]
    held += by_pair(pairs, far, per_peer)

    def body(head):
        both = summed[head]
        attended = both[:tokens] - owned(head, per_peer, here, held) * both[tokens:]
        write_rows(attended, head, heads, tokens, gain, out_wide)

    each_head(heads, body)
    out[...] = out_wide[...].astype(out.dtype)


def finish(peers, heads, tokens, weights, partial, known, gain, *refs):
    here, _, straight, crossed = sources(peers)
    last, pairs, (out, out_wide) = refs[: len(crossed)], refs[len(crossed) : -2], refs[-2:]
    per_peer = heads // peers
    held = [(stamped(ref, heads * tokens, per_peer), source, "pack") for ref, source in zip(last, crossed)]
    held += by_pair(pairs, (straight, crossed), per_peer) if pairs else []

    def body(head):
        both = partial[head] + weighted(
            [weights[i, head] for i in range(len(last))], [head_rows(ref, head, tokens) for ref in last]
        )
        second = known[head, 0:1, :]
        if held:
            second += owned(head, per_peer, here, held)
        attended = both[:tokens] - second * both[tokens:]
        write_rows(attended, head, heads, tokens, gain, out_wide)

    each_head(heads, body)
    out[...] = out_wide[...].astype(out.dtype)


def hold(*refs):
    pass


def kernel(body, outs, scratch, fetched=False, keep=False, aliases=None):
    space = pl.BlockSpec(memory_space=pltpu.VMEM)
    held = sum(4 * math.prod(s.shape) for s in scratch if s.dtype == jnp.float32)
    held += sum(math.prod(o.shape) * o.dtype.itemsize for o in jax.tree.leaves(outs))

    def call(*args):
        limit = SPARE_BYTES + held + sum(a.size * a.dtype.itemsize for a in args)
        if fetched or keep:
            args = [pltpu.with_memory_space_constraint(a, pltpu.HBM if fetched else pltpu.VMEM) for a in args]
        return pl.pallas_call(
            body,
            out_shape=outs,
            in_specs=[pl.BlockSpec(memory_space=pltpu.SMEM) if a.ndim == 1 else space for a in args],
            out_specs=jax.tree.map(lambda _: space, outs),
            scratch_shapes=scratch,
            input_output_aliases={i: i for i in range(len(args))} if keep else aliases or {},
            compiler_params=pltpu.CompilerParams(vmem_limit_bytes=limit),
        )(*args)

    return call


def on_device(query_rows, key_rows, value_rows, map_weight, head_gain):
    peers = lax.axis_size("sp")
    _, tokens, heads, width = query_rows.shape
    cores = CORES if peers % CORES == 0 else 1
    chips = peers // cores
    rows = tokens * heads

    def turn(x, by):
        return lax.ppermute(x, "sp", [(i, (i + by * cores) % peers) for i in range(peers)])

    def swap(x):
        return lax.ppermute(x, "sp", [(i, i // cores * cores + cores - 1 - i % cores) for i in range(peers)])

    def flat(x):
        return x.reshape(rows, width)

    f32 = lambda *s: jax.ShapeDtypeStruct(s, jnp.float32)
    bf16 = lambda *s: jax.ShapeDtypeStruct(s, jnp.bfloat16)
    wide = lambda n: pltpu.VMEM((n, rows, width), jnp.float32)
    both = (heads, 2 * tokens, tokens)
    shift = range(1, chips)
    n_near, n_far, n_last = cores, chips - 1, (chips - 1) * (cores - 1)

    chip = lax.axis_index("sp") // cores
    packs = (bf16(rows, width), bf16(rows + heads // peers * PACK, width))

    def sender():
        return kernel(functools.partial(pack, heads, tokens), packs, [wide(2)])(flat(key_rows), flat(value_rows))

    def receiver():
        return kernel(blank if chips > 2 else hold, packs, [])()

    key_pack, value_pack = lax.cond(chip < chips - 1, sender, receiver)
    key_far = [turn(key_pack, r) for r in shift]
    value_pack, tile = kernel(
        functools.partial(stamp, rows), (packs[1], f32(heads // peers, 8, width)), [], aliases={1: 0}
    )(map_weight, value_pack)
    value_far = [turn(value_pack, r) for r in shift]
    tiles = [tile] + ([swap(tile)] if cores > 1 else [])
    key_near = [swap(key_rows)] if cores > 1 else []
    value_near = [swap(value_rows)] if cores > 1 else []
    stacked, key_heads, value_heads, gain_tile = kernel(
        functools.partial(prepare, heads, tokens),
        (bf16(heads, 2 * tokens, width), bf16(rows, width), bf16(rows, width), f32(8, width)),
        [wide(3)],
        fetched=True,
    )(flat(query_rows), flat(key_rows), flat(value_rows), head_gain.reshape(1, -1))
    near_raised, near_level, gain_tile, pair = kernel(
        functools.partial(near_scores, peers, heads, tokens),
        (bf16(n_near, *both), f32(*both), f32(8, width), f32(n_near, heads // peers, 8, width)),
        [wide(max(cores - 1, 1))],
    )(stacked, key_heads, gain_tile, *tiles, *map(flat, key_near))
    pairs = [turn(pair, r) for r in shift]
    key_last = [swap(x) for x in key_far] if cores > 1 else []
    far_raised, level, summed, gain_tile, pair_tile = kernel(
        functools.partial(straight_scores, peers, heads, tokens, (cores - 1, n_near)),
        (
            bf16(n_far, *both), f32(*both), f32(heads, 2 * tokens, width), f32(8, width), f32(*pair.shape),
        ),
        [wide(max(cores - 1, 1))],
    )(stacked, near_raised, near_level, gain_tile, pair, value_heads, *map(flat, value_near), *key_far)

    def stay(*arrays):
        return kernel(hold, tuple(jax.ShapeDtypeStruct(x.shape, x.dtype) for x in arrays), [], keep=True)(*arrays)

    middle = chips > 2
    arrived = stay(*value_far, *key_last, *(pairs if middle else ()))
    value_far, key_last, late = arrived[:n_far], arrived[n_far : n_far + n_last], arrived[n_far + n_last :]

    def later_chip():
        value_last = [swap(x) for x in value_far] if cores > 1 else []
        weights, partial, known = kernel(
            functools.partial(last_scores, peers, heads, tokens),
            (bf16(n_last, *both), f32(heads, 2 * tokens, width), f32(heads, 8, width)),
            [],
        )(stacked, summed, level, far_raised, pair_tile, *value_far, *key_last)
        return kernel(
            functools.partial(finish, peers, heads, tokens),
            bf16(rows, width),
            [pltpu.VMEM((rows, width), jnp.float32)],
        )(weights, partial, known, gain_tile, *value_last, *late)

    def no_rows():
        return kernel(hold, bf16(rows, width), [])()

    mixed = lax.cond(chip > 0, later_chip, no_rows)
    mixed, *pairs = stay(mixed, *pairs)

    def first_chip():
        return kernel(
            functools.partial(finish_near, peers, heads, tokens),
            bf16(rows, width),
            [pltpu.VMEM((rows, width), jnp.float32)],
        )(summed, gain_tile, pair_tile, *pairs)

    mixed = lax.cond(chip > 0, lambda: mixed, first_chip)
    return mixed.reshape(query_rows.shape)


def solution(mesh):
    rows = P("dp", "sp", None, None)

    return jax.shard_map(
        on_device,
        mesh=mesh,
        in_specs=(rows, rows, rows, P("sp"), P()),
        out_specs=rows,
        check_vma=False,
    )
```

```python
import functools
import math

import jax
import jax.numpy as jnp
from jax import lax
from jax.experimental import pallas as pl
from jax.experimental.pallas import tpu as pltpu
from jax.sharding import PartitionSpec as P

QK = 64
SEGMENT = 64
CORES = 2
EXP_SCALE = math.log2(math.e) * QK ** (-0.5)
SPARE_BYTES = 2 << 20
PACK = 16
PARTS = 3
PIECES = 1
NT = (((1,), (1,)), ((), ()))


def each_head(heads, body):
    if heads <= 8:
        for head in range(heads):
            body(head)
    else:
        lax.fori_loop(0, heads, lambda head, c: (body(head), c)[1], 0)


def sources(peers):
    here = lax.axis_index("sp")
    cores = CORES if peers % CORES == 0 else 1
    chips = peers // cores
    chip, core = here // cores, here % cores
    straight = [lax.rem(chip + chips - r, chips) * cores + core for r in range(chips)]
    crossed = [lax.rem(chip + chips - r, chips) * cores + cores - 1 - core for r in range(chips)]
    if cores == 1:
        return here, [here], straight[1:], []
    return here, [here, crossed[0]], straight[1:], crossed[1:]


def widen(refs, wide):
    for i, ref in enumerate(refs):
        wide[i] = ref[...].astype(jnp.float32)
    return [wide.at[i] for i in range(len(refs))]


def split_rows(ref, head, heads, tokens):
    return ref[pl.ds(head, tokens, stride=heads), :].astype(jnp.bfloat16)


def head_rows(ref, head, tokens):
    return ref[pl.ds(head * tokens, tokens), :]


def hide(scores, here, source, tokens):
    queries = here * tokens + lax.rem(lax.broadcasted_iota(jnp.int32, scores.shape, 0), tokens)
    keys = source * tokens + lax.broadcasted_iota(jnp.int32, scores.shape, 1)
    return jnp.where(keys // SEGMENT <= queries // SEGMENT, scores, -jnp.inf)


def weigh(stacked, keys, srcs, here, tokens, floor):
    scores = [
        hide(lax.dot_general(stacked, key, NT, preferred_element_type=jnp.float32), here, source, tokens)
        for key, source in zip(keys, srcs)
    ]
    top = jnp.max(functools.reduce(jnp.maximum, scores), axis=1, keepdims=True)
    top = jnp.broadcast_to(top, scores[0].shape)
    if floor is not None:
        top = jnp.maximum(top, floor)
    raised = [jnp.exp2((block - top) * EXP_SCALE) for block in scores]
    total = jnp.sum(functools.reduce(jnp.add, raised), axis=1, keepdims=True)
    return top, raised, jnp.broadcast_to(total, scores[0].shape)


def weighted(blocks, values):
    return functools.reduce(
        jnp.add, [jnp.dot(block, value, preferred_element_type=jnp.float32) for block, value in zip(blocks, values)]
    )


def prepare(heads, tokens, query, key, value, gain, stacked, key_heads, value_heads, gain_tile, wide):
    query_wide, key_wide, value_wide = widen((query, key, value), wide)

    def body(head):
        rows = split_rows(query_wide, head, heads, tokens)
        first = lax.broadcasted_iota(jnp.int32, rows.shape, 1) < QK
        zero = jnp.zeros_like(rows)
        stacked[head] = jnp.concatenate([jnp.where(first, rows, zero), jnp.where(first, zero, rows)], axis=0)
        key_heads[pl.ds(head * tokens, tokens), :] = split_rows(key_wide, head, heads, tokens)
        value_heads[pl.ds(head * tokens, tokens), :] = split_rows(value_wide, head, heads, tokens)

    each_head(heads, body)
    gain_tile[...] = jnp.broadcast_to(gain[...], gain_tile.shape)


def pack(heads, tokens, key, value, key_pack, value_pack, wide):
    key_wide, value_wide = widen((key, value), wide)

    def body(head):
        key_pack[pl.ds(head * tokens, tokens), :] = split_rows(key_wide, head, heads, tokens)
        value_pack[pl.ds(head * tokens, tokens), :] = split_rows(value_wide, head, heads, tokens)

    each_head(heads, body)


def blank(key_pack, value_pack):
    for ref in (key_pack, value_pack):
        ref[...] = jnp.zeros_like(ref)


def stamp(rows, map_weight, value_in, value_pack, tile):
    value_pack[pl.ds(0, rows), :] = value_in[pl.ds(0, rows), :]
    for own in range(tile.shape[0]):
        rest = jnp.full((PACK, value_pack.shape[1]), map_weight[own])
        tile[own] = rest[: tile.shape[1]]
        row = lax.broadcasted_iota(jnp.int32, rest.shape, 0)
        packed = jnp.zeros_like(rest)
        for part in range(PARTS):
            piece = rest.astype(jnp.bfloat16).astype(jnp.float32)
            packed = jnp.where(row == part, piece, packed)
            rest = rest - piece
        value_pack[pl.ds(rows + own * PACK, PACK), :] = packed.astype(jnp.bfloat16)


def stamped(value_pack, rows, per_peer):
    found = []
    for own in range(per_peer):
        parts = value_pack[pl.ds(rows + own * PACK, PACK), :].astype(jnp.float32)
        found.append(sum(parts[i : i + 1] for i in range(PARTS)))
    return found


def near_scores(peers, heads, tokens, stacked, key_heads, gain, *refs):
    here, near, _, _ = sources(peers)
    tiles, keys = refs[: len(near)], refs[len(near) : -5]
    raised, level, gain_out, pair, wide = refs[-5:]
    keys_wide = widen(keys, wide)
    gain_out[...] = gain[...]
    for i, tile in enumerate(tiles):
        pair[i] = tile[...]

    def body(head):
        blocks = [head_rows(key_heads, head, tokens)] + [split_rows(ref, head, heads, tokens) for ref in keys_wide]
        peak, blocks, mass = weigh(stacked[head], blocks, near, here, tokens, None)
        inverse = 1.0 / mass
        level[head] = peak + jnp.log(mass) * QK**0.5
        for i, block in enumerate(blocks):
            raised[i, head] = (block * inverse).astype(jnp.bfloat16)

    each_head(heads, body)


def straight_scores(peers, heads, tokens, counts, stacked, near_raised, near_level, gain, pair, value_heads, *refs):
    here, _, straight, _ = sources(peers)
    n_side, n_near = counts
    values, keys = refs[:n_side], refs[n_side:-6]
    raised, level, summed, gain_out, pair_out, value_wide = refs[-6:]
    gain_out[...] = gain[...]
    pair_out[...] = pair[...]
    values_wide = widen(values, value_wide)

    def body(head):
        blocks = [head_rows(ref, head, tokens) for ref in keys]
        peak, blocks, mass = weigh(stacked[head], blocks, straight, here, tokens, near_level[head])
        prior = jnp.exp2((near_level[head] - peak) * EXP_SCALE)
        mass = prior + mass
        inverse = 1.0 / mass
        level[head] = peak + jnp.log(mass) * QK**0.5
        for i, block in enumerate(blocks):
            raised[i, head] = (block * inverse).astype(jnp.bfloat16)
        near_values = [head_rows(value_heads, head, tokens)] + [split_rows(v, head, heads, tokens) for v in values_wide]
        summed[head] = weighted([near_raised[i, head] for i in range(n_near)], near_values) * (prior * inverse)

    each_head(heads, body)


def owned(head, per_peer, here, held):
    second = jnp.zeros_like(held[0][0][0])
    for rows, source, by in held:
        for own in range(per_peer):
            here_too = source * per_peer + own == head
            if by is not None:
                here_too = jnp.logical_and(here_too, (source < here) if by == "pack" else (source > here))
            second += jnp.where(here_too, rows[own], 0.0)
    return second


def tile_rows(tiles, i, per_peer):
    return [tiles[i, own, 0:1, :] for own in range(per_peer)]


def by_pair(pairs, side, per_peer):
    straight, crossed = side
    found = [(tile_rows(pair, 0, per_peer), source, "pair") for pair, source in zip(pairs, straight)]
    return found + [(tile_rows(pair, 1, per_peer), source, "pair") for pair, source in zip(pairs, crossed)]


def last_scores(peers, heads, tokens, stacked, summed, level, far_raised, near_pair, *refs):
    here, near, straight, crossed = sources(peers)
    values, keys, (weights, partial, second) = refs[: len(straight)], refs[len(straight) : -3], refs[-3:]
    per_peer = heads // peers
    held = [(tile_rows(near_pair, i, per_peer), source, None) for i, source in enumerate(near)]
    held += [(stamped(ref, heads * tokens, per_peer), source, "pack") for ref, source in zip(values, straight)]

    def body(head):
        second[head] = jnp.broadcast_to(owned(head, per_peer, here, held), second.shape[1:])
        blocks = [head_rows(ref, head, tokens) for ref in keys]
        peak, blocks, mass = weigh(stacked[head], blocks, crossed, here, tokens, level[head])
        prior = jnp.exp2((level[head] - peak) * EXP_SCALE)
        inverse = 1.0 / (prior + mass)
        for i, block in enumerate(blocks):
            weights[i, head] = (block * inverse).astype(jnp.bfloat16)
        far_values = [head_rows(ref, head, tokens) for ref in values]
        far = weighted([far_raised[i, head] for i in range(len(straight))], far_values)
        partial[head] = (summed[head] + far) * (prior * inverse)

    each_head(heads, body)


def write_rows(attended, head, heads, tokens, gain, out_wide):
    mean_square = jnp.mean(attended * attended, axis=1, keepdims=True)
    out_wide[pl.ds(head, tokens, stride=heads), :] = attended * lax.rsqrt(mean_square + 1e-06) * gain[0:1, :]


def write_out(out, out_wide, out_rows, sems):
    step = out_rows.shape[0] // PIECES
    moves = []
    for i in range(PIECES):
        piece = pl.ds(i * step, step)
        out_rows[piece, :] = out_wide[piece, :].astype(out_rows.dtype)
        moves.append(pltpu.make_async_copy(out_rows.at[piece], out.at[piece], sems.at[i]))
        moves[-1].start()
    for move in moves:
        move.wait()


def finish_near(peers, heads, tokens, summed, gain, near_pair, *refs):
    pairs, (out, out_wide, out_rows, sems) = refs[:-4], refs[-4:]
    here, near, *far = sources(peers)
    per_peer = heads // peers
    held = [(tile_rows(near_pair, i, per_peer), source, None) for i, source in enumerate(near)]
    held += by_pair(pairs, far, per_peer)

    def body(head):
        both = summed[head]
        attended = both[:tokens] - owned(head, per_peer, here, held) * both[tokens:]
        write_rows(attended, head, heads, tokens, gain, out_wide)

    each_head(heads, body)
    write_out(out, out_wide, out_rows, sems)


def finish(peers, heads, tokens, weights, partial, known, gain, *refs):
    here, _, straight, crossed = sources(peers)
    last, pairs, (out, out_wide, out_rows, sems) = refs[: len(crossed)], refs[len(crossed) : -4], refs[-4:]
    per_peer = heads // peers
    held = [(stamped(ref, heads * tokens, per_peer), source, "pack") for ref, source in zip(last, crossed)]
    held += by_pair(pairs, (straight, crossed), per_peer) if pairs else []

    def body(head):
        both = partial[head] + weighted(
            [weights[i, head] for i in range(len(last))], [head_rows(ref, head, tokens) for ref in last]
        )
        second = known[head, 0:1, :]
        if held:
            second += owned(head, per_peer, here, held)
        attended = both[:tokens] - second * both[tokens:]
        write_rows(attended, head, heads, tokens, gain, out_wide)

    each_head(heads, body)
    write_out(out, out_wide, out_rows, sems)


def hold(*refs):
    pass


def kernel(body, outs, scratch, fetched=False, keep=False, aliases=None, away=False):
    space = pl.BlockSpec(memory_space=pltpu.VMEM)
    held = sum(4 * math.prod(s.shape) for s in scratch if s.dtype == jnp.float32)
    held += sum(math.prod(o.shape) * o.dtype.itemsize for o in jax.tree.leaves(outs))

    def call(*args):
        limit = SPARE_BYTES + held + sum(a.size * a.dtype.itemsize for a in args)
        if fetched or keep:
            args = [pltpu.with_memory_space_constraint(a, pltpu.HBM if fetched else pltpu.VMEM) for a in args]
        return pl.pallas_call(
            body,
            out_shape=pltpu.HBM(outs.shape, outs.dtype) if away else outs,
            in_specs=[pl.BlockSpec(memory_space=pltpu.SMEM) if a.ndim == 1 else space for a in args],
            out_specs=jax.tree.map(lambda _: pl.BlockSpec(memory_space=pltpu.HBM) if away else space, outs),
            scratch_shapes=scratch,
            input_output_aliases={i: i for i in range(len(args))} if keep else aliases or {},
            compiler_params=pltpu.CompilerParams(vmem_limit_bytes=limit),
        )(*args)

    return call


def on_device(query_rows, key_rows, value_rows, map_weight, head_gain):
    peers = lax.axis_size("sp")
    _, tokens, heads, width = query_rows.shape
    cores = CORES if peers % CORES == 0 else 1
    chips = peers // cores
    rows = tokens * heads

    def turn(x, by):
        return lax.ppermute(x, "sp", [(i, (i + by * cores) % peers) for i in range(peers)])

    def swap(x):
        return lax.ppermute(x, "sp", [(i, i // cores * cores + cores - 1 - i % cores) for i in range(peers)])

    def flat(x):
        return x.reshape(rows, width)

    f32 = lambda *s: jax.ShapeDtypeStruct(s, jnp.float32)
    bf16 = lambda *s: jax.ShapeDtypeStruct(s, jnp.bfloat16)
    wide = lambda n: pltpu.VMEM((n, rows, width), jnp.float32)
    both = (heads, 2 * tokens, tokens)
    shift = range(1, chips)
    n_near, n_far, n_last = cores, chips - 1, (chips - 1) * (cores - 1)

    chip = lax.axis_index("sp") // cores
    packs = (bf16(rows, width), bf16(rows + heads // peers * PACK, width))

    def sender():
        return kernel(functools.partial(pack, heads, tokens), packs, [wide(2)])(flat(key_rows), flat(value_rows))

    def receiver():
        return kernel(blank if chips > 2 else hold, packs, [])()

    key_pack, value_pack = lax.cond(chip < chips - 1, sender, receiver)
    key_far = [turn(key_pack, r) for r in shift]
    value_pack, tile = kernel(
        functools.partial(stamp, rows), (packs[1], f32(heads // peers, 8, width)), [], aliases={1: 0}
    )(map_weight, value_pack)
    value_far = [turn(value_pack, r) for r in shift]
    tiles = [tile] + ([swap(tile)] if cores > 1 else [])
    key_near = [swap(key_rows)] if cores > 1 else []
    value_near = [swap(value_rows)] if cores > 1 else []
    stacked, key_heads, value_heads, gain_tile = kernel(
        functools.partial(prepare, heads, tokens),
        (bf16(heads, 2 * tokens, width), bf16(rows, width), bf16(rows, width), f32(8, width)),
        [wide(3)],
        fetched=True,
    )(flat(query_rows), flat(key_rows), flat(value_rows), head_gain.reshape(1, -1))
    near_raised, near_level, gain_tile, pair = kernel(
        functools.partial(near_scores, peers, heads, tokens),
        (bf16(n_near, *both), f32(*both), f32(8, width), f32(n_near, heads // peers, 8, width)),
        [wide(max(cores - 1, 1))],
    )(stacked, key_heads, gain_tile, *tiles, *map(flat, key_near))
    pairs = [turn(pair, r) for r in shift]
    key_last = [swap(x) for x in key_far] if cores > 1 else []
    far_raised, level, summed, gain_tile, pair_tile = kernel(
        functools.partial(straight_scores, peers, heads, tokens, (cores - 1, n_near)),
        (
            bf16(n_far, *both), f32(*both), f32(heads, 2 * tokens, width), f32(8, width), f32(*pair.shape),
        ),
        [wide(max(cores - 1, 1))],
    )(stacked, near_raised, near_level, gain_tile, pair, value_heads, *map(flat, value_near), *key_far)

    def stay(*arrays):
        return kernel(hold, tuple(jax.ShapeDtypeStruct(x.shape, x.dtype) for x in arrays), [], keep=True)(*arrays)

    middle = chips > 2
    writer = [
        pltpu.VMEM((rows, width), jnp.float32),
        pltpu.VMEM((rows, width), jnp.bfloat16),
        pltpu.SemaphoreType.DMA((PIECES,)),
    ]
    arrived = stay(*value_far, *key_last, *(pairs if middle else ()))
    value_far, key_last, late = arrived[:n_far], arrived[n_far : n_far + n_last], arrived[n_far + n_last :]

    def later_chip():
        value_last = [swap(x) for x in value_far] if cores > 1 else []
        weights, partial, known = kernel(
            functools.partial(last_scores, peers, heads, tokens),
            (bf16(n_last, *both), f32(heads, 2 * tokens, width), f32(heads, 8, width)),
            [],
        )(stacked, summed, level, far_raised, pair_tile, *value_far, *key_last)
        return kernel(
            functools.partial(finish, peers, heads, tokens),
            bf16(rows, width),
            writer,
            away=True,
        )(weights, partial, known, gain_tile, *value_last, *late)

    def no_rows():
        return kernel(hold, bf16(rows, width), [], away=True)()

    mixed = lax.cond(chip > 0, later_chip, no_rows)
    mixed, pairs = lax.optimization_barrier((mixed, pairs))
    pairs = stay(*pairs)

    def first_chip():
        return kernel(
            functools.partial(finish_near, peers, heads, tokens),
            bf16(rows, width),
            writer,
            away=True,
        )(summed, gain_tile, pair_tile, *pairs)

    mixed = lax.cond(chip > 0, lambda: mixed, first_chip)
    return mixed.reshape(query_rows.shape)


def solution(mesh):
    rows = P("dp", "sp", None, None)

    return jax.shard_map(
        on_device,
        mesh=mesh,
        in_specs=(rows, rows, rows, P("sp"), P()),
        out_specs=rows,
        check_vma=False,
    )
```
